32 devices in a mesh: sp: 4 (over z), fs: 4 (over y, core), tp: 2 (over x).
Axes of the slice: x: 2, y: 2, z: 4, core: 2. Of those that a mesh axis runs over, the one named last changes fastest.
Arguments:
- tokens: bfloat16 [4096, 2048], P(('fs', 'sp', 'tp')), parts along dimension 0, may hold values from -6 to 6
- norm_gain: bfloat16 [2048], replicated, may hold values from 0.099609375 to 1.8984375
- w_pool_in: bfloat16 [2048, 1024], P('sp', 'tp'), may hold values from -0.125 to 0.125
- w_query: bfloat16 [2048, 1024], P('sp', 'tp'), may hold values from -0.125 to 0.125
- w_key: bfloat16 [2048, 1024], P('sp', 'tp'), may hold values from -0.125 to 0.125
- w_value: bfloat16 [2048, 1024], P('sp', 'tp'), may hold values from -0.125 to 0.125
- w_gate: bfloat16 [2048, 1024], P('sp', 'tp'), may hold values from -0.125 to 0.125
- w_beta: bfloat16 [2048, 8], replicated, may hold values from -0.125 to 0.125
- w_decay: bfloat16 [2048, 8], replicated, may hold values from -0.5 to 0.5
- conv_weight: float32 [3, 4, 1024], P(None, None, 'tp'), may hold values from -3 to 3
- a_log: float32 [8], P('tp'), may hold values from -20 to -1.7, as said below
- decay_extra: float32 [4096, 8], P(('fs', 'sp'), 'tp'), parts along dimension 0, may hold values from -1.4 to 0
- w_mix: bfloat16 [8, 128, 128], P('tp'), may hold values from -0.5 to 0.5
- pool_scale: float32 [1024], P('tp'), may hold values from 0.1 to 1.9
- delta_gain: float32 [128], replicated, may hold values from 0.1 to 1.9
- w_out_pool: bfloat16 [1024, 2048], P('tp', 'sp'), may hold values from -0.125 to 0.125
- w_out_delta: bfloat16 [1024, 2048], P('tp', 'sp'), may hold values from -0.125 to 0.125
Outputs:
- mixed: bfloat16 [4096, 2048], P(('fs', 'sp', 'tp')), parts along dimension 0
The draws below stay inside these ranges and needn't reach their ends.
There are 4 independent parts, one for each index of `fs`. The reference program is written for one: setup_inputs(seed, part) draws one part's arguments, and reference() takes and returns one part's arrays. A program takes and returns all parts, laid end to end along the dimension named above; an argument that names none is the same for every part. Nothing has to cross between parts.
Inputs may be any that keep to these rules, and one draw needn't show every extreme that they name: `a_log`: logarithm of each head's base decay rate.
All inputs are finite; a program needn't handle non-finite values.
Results may differ from the reference program's by a relative error of at most 0.018.
Values may be sent and summed in bfloat16 or wider, within the bound.
A program may use at most 64 MiB of HBM per device.

```python
import jax
import jax.numpy as jnp
from jax import lax

D = 2048
POOL_GROUPS = 8
GROUP_DIM = 128
DN_HEADS = 8
HEAD_DIM = 128
CONV = 4
BLOCK = 64
SP_TOK = 256
POOL_WIDTH = 1024
DN_WIDTH = 1024
SEQ = 1024
N_TP = 2


def draw_a_log(key, part):
    chooser, slow_key, fast_key = jax.random.split(jax.random.fold_in(key, 11), 3)
    fast_share = 0.5
    fast = jax.random.uniform(chooser, (DN_HEADS,), jnp.float32) < fast_share
    slow_rate = jnp.exp(jax.random.uniform(slow_key, (DN_HEADS,), jnp.float32, jnp.log(0.05), jnp.log(0.2))) / SEQ
    fast_rate = jax.random.uniform(fast_key, (DN_HEADS,), jnp.float32, 1.0 / 16.0, 1.0 / 6.0)
    return jnp.log(jnp.where(fast, fast_rate, slow_rate)).astype(jnp.float32)


def draw_decay_extra(key, part):
    rate_key, position_seed, depth_key = jax.random.split(jax.random.fold_in(key, 23), 3)
    rates = jnp.exp(jax.random.uniform(rate_key, (SEQ // SP_TOK, DN_HEADS), jnp.float32, jnp.log(0.1), jnp.log(0.6))) / SEQ
    starting_shift = -jnp.repeat(rates, SP_TOK, axis=0)
    places = jax.random.randint(position_seed, (2, DN_HEADS), 0, SEQ)
    layer_ordinal = jax.random.uniform(depth_key, (2, DN_HEADS), jnp.float32, 0.22, 0.69)
    positions = jnp.arange(SEQ, dtype=jnp.int32)
    agreeing_tally = (positions[:, None, None] == places[None, :, :]).astype(jnp.float32)
    window_bundles = -jnp.sum(agreeing_tally * layer_ordinal[None, :, :], axis=1)
    return (starting_shift + window_bundles).astype(jnp.float32)


def shard_levels(own_key, shape, shards, smallest, high):
    loudness = 1.0
    for position, parts in shards:
        heights = jax.random.uniform(jax.random.fold_in(jax.random.fold_in(own_key, 6), position), (parts,), jnp.float32, smallest / len(shards), high / len(shards))
        loudness = loudness * jnp.repeat(jnp.exp(heights), shape[position] // parts).reshape((-1,) + (1,) * (len(shape) - 1 - position))
    return loudness


def centred(stream_key, shape, scale, most, shards=(), kind=jnp.bfloat16):
    values = scale * jax.random.normal(stream_key, shape, jnp.float32)
    if shards:
        values = values * shard_levels(stream_key, shape, shards, -0.22, 0.18)
    return jnp.clip(values, -most, most).astype(kind)


def setup_inputs(seed: int = 0, part: int = 0) -> dict:
    seeds = jax.random.split(jax.random.key(seed), 18)
    part_keys = jax.random.split(jax.random.fold_in(seeds[17], part), 18)
    return {
        "tokens": centred(part_keys[0], (SEQ, D), 1.0, 6.0, ((0, 8),)),
        "norm_gain": jnp.clip(1.0 + 0.18 * jax.random.normal(seeds[1], (D,), jnp.float32), 0.099609375, 1.8984375).astype(jnp.bfloat16),
        "w_pool_in": centred(seeds[2], (D, POOL_WIDTH), D ** -0.5, 0.125, ((0, 4), (1, 2))),
        "w_query": centred(seeds[3], (D, DN_WIDTH), D ** -0.5, 0.125, ((0, 4), (1, 2))),
        "w_key": centred(seeds[4], (D, DN_WIDTH), D ** -0.5, 0.125, ((0, 4), (1, 2))),
        "w_value": centred(seeds[5], (D, DN_WIDTH), D ** -0.5, 0.125, ((0, 4), (1, 2))),
        "w_gate": centred(seeds[6], (D, DN_WIDTH), D ** -0.5, 0.125, ((0, 4), (1, 2))),
        "w_beta": centred(seeds[7], (D, DN_HEADS), D ** -0.5, 0.125),
        "w_decay": centred(seeds[8], (D, DN_HEADS), (D // 16) ** -0.5, 0.5),
        "conv_weight": centred(seeds[9], (3, CONV, DN_WIDTH), CONV ** -0.5, 3.0, ((2, 2),), jnp.float32),
        "a_log": draw_a_log(jax.random.fold_in(seeds[17], 71), part),
        "decay_extra": draw_decay_extra(jax.random.fold_in(jax.random.fold_in(seeds[17], part), 71), part),
        "w_mix": centred(seeds[12], (POOL_GROUPS, GROUP_DIM, GROUP_DIM), GROUP_DIM ** -0.5, 0.5, ((0, 2),)),
        "pool_scale": jnp.clip(1.0 + 0.18 * jax.random.normal(seeds[13], (POOL_WIDTH,), jnp.float32), 0.1, 1.9),
        "delta_gain": jnp.clip(1.0 + 0.18 * jax.random.normal(seeds[14], (HEAD_DIM,), jnp.float32), 0.1, 1.9),
        "w_out_pool": centred(seeds[15], (POOL_WIDTH, D), (POOL_WIDTH + DN_WIDTH) ** -0.5, 0.125, ((0, 2), (1, 4))),
        "w_out_delta": centred(seeds[16], (DN_WIDTH, D), (POOL_WIDTH + DN_WIDTH) ** -0.5, 0.125, ((0, 2), (1, 4))),
    }


eps = 1e-06
windows = (2, 4, 8, 16)
highest = lax.Precision.HIGHEST

def rms_rows(values, gain):
    floats = values.astype(jnp.float32)
    scale = lax.rsqrt(lax.optimization_barrier(jnp.mean(floats * floats, axis=-1, keepdims=True)) + eps)
    return (floats * scale * gain.astype(jnp.float32)).astype(jnp.bfloat16)

def unit_rows(values):
    return values * lax.rsqrt(lax.optimization_barrier(jnp.sum(values * values, axis=-1, keepdims=True)) + eps)

def block_terms(query, keys, values, log_gate, strength, block):
    heads, length, width = keys.shape
    count = length // block

    def split(tensor):
        return tensor.reshape(heads, count, block, tensor.shape[-1])
    query_part, key_part, value_part = (split(query), split(keys), split(values))
    gate_cum = jnp.cumsum(log_gate.reshape(heads, count, block), axis=-1)
    beta_part = strength.reshape(heads, count, block)[..., None]
    lower_mask = jnp.tril(jnp.ones((block, block), dtype=bool))
    strict_mask = jnp.tril(jnp.ones((block, block), dtype=bool), k=-1)
    gaps = gate_cum[..., :, None] - gate_cum[..., None, :]
    decay_tab = jnp.where(lower_mask, jnp.exp(jnp.where(lower_mask, gaps, 0.0)), 0.0)
    key_scaled_beta = key_part * beta_part
    value_beta = value_part * beta_part
    corr_lower = jnp.where(strict_mask, jnp.einsum('hnid,hnjd->hnij', key_scaled_beta, key_part, precision=highest) * decay_tab, 0.0)
    identity = jnp.eye(block, dtype=jnp.float32)
    inverse = lax.linalg.triangular_solve(identity + corr_lower, jnp.broadcast_to(identity, corr_lower.shape), left_side=True, lower=True)
    fixed_values = jnp.einsum('hnij,hnjd->hnid', inverse, value_beta, precision=highest)
    key_weights = jnp.einsum('hnij,hnjd->hnid', inverse, key_scaled_beta * jnp.exp(gate_cum)[..., None], precision=highest)
    scores = jnp.where(lower_mask, jnp.einsum('hnid,hnjd->hnij', query_part, key_part, precision=highest) * decay_tab, 0.0)
    key_decayed = key_part * jnp.exp(gate_cum[..., -1:] - gate_cum)[..., None]
    query_gated = query_part * jnp.exp(gate_cum)[..., None]
    terms = (query_gated, key_decayed, fixed_values, key_weights, scores, gate_cum[..., -1])
    return tuple((jnp.moveaxis(tensor, 1, 0) for tensor in terms))

def carry_step(state, inputs):
    query_gated, key_decayed, fixed_values, key_weights, scores, last_gate = inputs
    fresh = fixed_values - jnp.einsum('hcd,hde->hce', key_weights, state, precision=highest)
    output = jnp.einsum('hcd,hde->hce', query_gated, state, precision=highest) + jnp.einsum('hij,hje->hie', scores, fresh, precision=highest)
    state = state * jnp.exp(last_gate)[:, None, None] + jnp.einsum('hcd,hce->hde', key_decayed, fresh, precision=highest)
    return (state, output)

def reference(tokens, norm_gain, w_pool_in, w_query, w_key, w_value, w_gate, w_beta, w_decay, conv_weight, a_log, decay_extra, w_mix, pool_scale, delta_gain, w_out_pool, w_out_delta):
    norm_result = rms_rows(tokens, norm_gain)

    def project(weight):
        return jnp.dot(norm_result.astype(jnp.float32), weight.astype(jnp.float32), preferred_element_type=jnp.float32).astype(jnp.bfloat16)
    pool_in = project(w_pool_in)
    query_raw = project(w_query)
    key_raw = project(w_key)
    value_raw = project(w_value)
    gate_raw = project(w_gate)
    beta_pre = jnp.dot(norm_result.astype(jnp.float32), w_beta.astype(jnp.float32), preferred_element_type=jnp.float32)
    forget_logits = jnp.dot(norm_result.astype(jnp.float32), w_decay.astype(jnp.float32), preferred_element_type=jnp.float32)
    source_rows = pool_in.astype(jnp.float32)
    running = jnp.concatenate([jnp.zeros((1, POOL_WIDTH), jnp.float32), jnp.cumsum(source_rows, axis=0)], axis=0)
    group = (jnp.arange(POOL_WIDTH) // GROUP_DIM).astype(jnp.int32)
    span = (2 ** (1 + group % 4)).astype(jnp.int32)
    window_sum = jnp.zeros((SEQ, POOL_WIDTH), jnp.float32)
    for width in windows:
        lagged = jnp.concatenate([jnp.zeros((width - 1, POOL_WIDTH), jnp.float32), running[:SEQ - width + 1]], axis=0)
        window_sum = window_sum + jnp.where(span[None, :] == width, running[1:] - lagged, 0.0)
    positions = jnp.arange(SEQ).astype(jnp.int32)
    counts = jnp.minimum(positions[:, None] + 1, span[None, :]).astype(jnp.float32)
    pooled = (window_sum / counts - source_rows).astype(jnp.bfloat16)
    mixed_pool = jnp.einsum('sgc,gcd->sgd', pooled.reshape(SEQ, POOL_GROUPS, GROUP_DIM).astype(jnp.float32), w_mix.astype(jnp.float32), precision=highest)
    pool_out = (mixed_pool.reshape(SEQ, POOL_WIDTH) * pool_scale).astype(jnp.bfloat16)
    stacked = jnp.concatenate([query_raw, key_raw, value_raw], axis=1).astype(jnp.float32)
    kernel = jnp.transpose(conv_weight, (1, 0, 2)).reshape(CONV, 3 * DN_WIDTH)
    padded = jnp.concatenate([jnp.zeros((CONV - 1, 3 * DN_WIDTH), jnp.float32), stacked], axis=0)
    conv = jnp.zeros((SEQ, 3 * DN_WIDTH), jnp.float32)
    for tap in range(CONV):
        conv = conv + padded[tap:tap + SEQ] * kernel[tap]
    after_silu = jax.nn.silu(conv)

    def heads_first(tensor):
        return jnp.transpose(tensor.reshape(SEQ, DN_HEADS, HEAD_DIM), (1, 0, 2))
    query = unit_rows(heads_first(after_silu[:, :DN_WIDTH])) * HEAD_DIM ** (-0.5)
    keys = unit_rows(heads_first(after_silu[:, DN_WIDTH:2 * DN_WIDTH]))
    values = heads_first(after_silu[:, 2 * DN_WIDTH:])
    strength = jax.nn.sigmoid(beta_pre).T
    log_gate = (-jnp.exp(a_log)[None, :] * jax.nn.softplus(forget_logits) + decay_extra).T
    terms = block_terms(query, keys, values, log_gate, strength, BLOCK)
    _, outputs = lax.scan(carry_step, jnp.zeros((DN_HEADS, HEAD_DIM, HEAD_DIM), jnp.float32), terms)
    attended = jnp.transpose(outputs, (1, 0, 2, 3)).reshape(DN_HEADS, SEQ, HEAD_DIM)
    normal_out = attended * lax.rsqrt(lax.optimization_barrier(jnp.mean(attended * attended, axis=-1, keepdims=True)) + eps) * delta_gain
    gated = normal_out * jax.nn.silu(heads_first(gate_raw.astype(jnp.float32)))
    delta_out = jnp.transpose(gated, (1, 0, 2)).reshape(SEQ, DN_WIDTH).astype(jnp.bfloat16)
    pool_cols = POOL_WIDTH // N_TP
    delta_cols = DN_WIDTH // N_TP
    total = jnp.zeros((SEQ, D), jnp.float32)
    for lane in range(N_TP):
        value_partial_rows = jnp.dot(pool_out[:, lane * pool_cols:(lane + 1) * pool_cols].astype(jnp.float32), w_out_pool[lane * pool_cols:(lane + 1) * pool_cols].astype(jnp.float32), preferred_element_type=jnp.float32)
        value_partial_rows = value_partial_rows + jnp.dot(delta_out[:, lane * delta_cols:(lane + 1) * delta_cols].astype(jnp.float32), w_out_delta[lane * delta_cols:(lane + 1) * delta_cols].astype(jnp.float32), preferred_element_type=jnp.float32)
        total = total + lax.optimization_barrier(value_partial_rows.astype(jnp.bfloat16)).astype(jnp.float32)
    return total.astype(jnp.bfloat16)
```

```python
import functools

import jax
import jax.numpy as jnp
from jax import lax
from jax.experimental import pallas as pl
from jax.experimental.pallas import tpu as pltpu
from jax.sharding import PartitionSpec as P

BLOCK = 64


eps = 1e-06
windows = (2, 4, 8, 16)
tail_rows = 15
highest = lax.Precision.HIGHEST


MESH = pl.DeviceIdType.MESH
halo = 16


def share_bits(n_fs):
    if n_fs & (n_fs - 1):
        return []
    return [n_fs >> (k + 1) for k in range(n_fs.bit_length() - 1)]


class Gather:
    def __init__(self, n_sp, n_fs, wbuf, z_s, z_r, f_s, f_r):
        self.n_sp, self.bits = n_sp, share_bits(n_fs)
        self.wbuf, self.z_s, self.z_r, self.f_s, self.f_r = wbuf, z_s, z_r, f_s, f_r
        self.sp, self.fs = lax.axis_index("sp"), lax.axis_index("fs")
        self.pieces = 2 ** len(self.bits)
        self.mine = self.fs if self.bits else 0 * self.fs
        self.depth = wbuf.shape[2] // self.pieces

    def partner(self, bit):
        return self.fs + bit * (1 - 2 * (self.fs // bit % 2))

    def mask_of(self, m, index):
        for i, bit in enumerate(self.bits):
            if m >> i & 1:
                index = index + bit * (1 - 2 * (index // bit % 2))
        return index

    def piece(self, w, src, index):
        return self.wbuf.at[w, src, pl.ds(pl.multiple_of(index * self.depth, self.depth), self.depth)]

    def z_copy(self, w, d, src):
        ref = self.piece(w, src, self.mine)
        return pltpu.make_async_remote_copy(
            src_ref=ref, dst_ref=ref, send_sem=self.z_s.at[w, d - 1], recv_sem=self.z_r.at[w, d - 1],
            device_id={"sp": lax.rem(self.sp + d, self.n_sp)}, device_id_type=MESH)

    def source(self, d):
        return lax.rem(self.sp - d + self.n_sp, self.n_sp)

    def f_copy(self, w, d, k, m):
        slot = 2 ** k - 1 + m
        ref = self.piece(w, self.source(d), self.mask_of(m, self.mine))
        return pltpu.make_async_remote_copy(
            src_ref=ref, dst_ref=ref, send_sem=self.f_s.at[w, d - 1, slot], recv_sem=self.f_r.at[w, d - 1, slot],
            device_id={"fs": self.partner(self.bits[k])}, device_id_type=MESH)

    def send(self, w):
        def body(d, c):
            self.z_copy(w, d, self.sp).start()
            return c
        lax.fori_loop(1, self.n_sp, body, 0)

    def arrive_z(self, w, d):
        self.z_copy(w, d, self.source(d)).wait_recv()
        for k in range(len(self.bits)):
            self.f_copy(w, d, k, 0).start()

    def arrive_f(self, w, d, k):
        for m in range(2 ** k):
            self.f_copy(w, d, k, m).wait_recv()
            for later in range(k + 1, len(self.bits)):
                self.f_copy(w, d, later, m | 1 << k).start()

    def forward(self, w):
        last = self.n_sp - 1
        inner = len(self.bits) - 1

        def body(d, c):
            self.arrive_z(w, d)
            for k in range(inner):
                if w == 0:
                    @pl.when(d > 1)
                    def _():
                        self.arrive_f(w, d - 1, k)
                else:
                    @pl.when(d > 1)
                    def _():
                        self.arrive_f(w, d - 1, k)

                    @pl.when(d == 1)
                    def _():
                        self.arrive_f(w - 1, last, k)
            return c
        lax.fori_loop(1, self.n_sp, body, 0)

    def flush(self, w):
        for k in range(len(self.bits) - 1):
            self.arrive_f(w, self.n_sp - 1, k)

    def finish(self, w):
        if self.bits:
            def body(d, c):
                self.arrive_f(w, d, len(self.bits) - 1)
                return c
            lax.fori_loop(1, self.n_sp, body, 0)

    def drain(self, w):
        def body(d, c):
            self.z_copy(w, d, self.sp).wait_send()
            for k in range(len(self.bits)):
                for m in range(2 ** k):
                    self.f_copy(w, d, k, m).wait_send()
            return c
        lax.fori_loop(1, self.n_sp, body, 0)


def enter(n_sp, n_fs, n_tp):
    sp, fs, tp = (lax.axis_index(a) for a in ("sp", "fs", "tp"))
    barrier = pltpu.get_barrier_semaphore()
    bits = share_bits(n_fs)
    for d in range(1, n_sp):
        pl.semaphore_signal(barrier, inc=1, device_id={"sp": lax.rem(sp + d, n_sp)}, device_id_type=MESH)
    for bit in bits:
        pl.semaphore_signal(barrier, inc=1, device_id={"fs": fs + bit * (1 - 2 * (fs // bit % 2))}, device_id_type=MESH)
    for d in range(1, n_tp):
        pl.semaphore_signal(barrier, inc=1, device_id={"tp": lax.rem(tp + d, n_tp)}, device_id_type=MESH)
    pl.semaphore_wait(barrier, n_sp - 1 + len(bits) + n_tp - 1)


def gather_tokens(n_sp, n_tp, tokbuf, rows, tok_s, tok_r, halo_s, halo_r):
    sp, tp = lax.axis_index("sp"), lax.axis_index("tp")

    def tok_copy(d, owner):
        ref = tokbuf.at[pl.ds(pl.multiple_of(halo + owner * rows, 16), rows)]
        return pltpu.make_async_remote_copy(
            src_ref=ref, dst_ref=ref, send_sem=tok_s.at[d - 1], recv_sem=tok_r.at[d - 1],
            device_id={"tp": lax.rem(tp + d, n_tp)}, device_id_type=MESH)

    def halo_next():
        return pltpu.make_async_remote_copy(
            src_ref=tokbuf.at[pl.ds(n_tp * rows, halo)], dst_ref=tokbuf.at[pl.ds(0, halo)],
            send_sem=halo_s.at[0], recv_sem=halo_r.at[0],
            device_id={"sp": lax.rem(sp + 1, n_sp)}, device_id_type=MESH)

    def halo_side(d):
        ref = tokbuf.at[pl.ds(0, halo)]
        return pltpu.make_async_remote_copy(
            src_ref=ref, dst_ref=ref, send_sem=halo_s.at[d], recv_sem=halo_r.at[d],
            device_id={"tp": lax.rem(tp + d, n_tp)}, device_id_type=MESH)

    end = n_tp - 1

    def start():
        for d in range(1, n_tp):
            tok_copy(d, tp).start()

        @pl.when(jnp.logical_and(tp == end, sp < n_sp - 1))
        def _():
            halo_next().start()

        @pl.when(sp == 0)
        def _():
            tokbuf[0:halo, :] = jnp.zeros((halo, tokbuf.shape[1]), tokbuf.dtype)

    def finish():
        @pl.when(jnp.logical_and(tp == end, sp > 0))
        def _():
            halo_next().wait_recv()
            for d in range(1, n_tp):
                halo_side(d).start()
        for d in range(1, n_tp):
            tok_copy(d, lax.rem(tp - d + n_tp, n_tp)).wait_recv()

        @pl.when(jnp.logical_and(tp < end, sp > 0))
        def _():
            for d in range(1, n_tp):
                @pl.when(tp == d - 1)
                def _():
                    halo_side(d).wait_recv()

    def drain():
        for d in range(1, n_tp):
            tok_copy(d, tp).wait_send()

        @pl.when(jnp.logical_and(tp == end, sp < n_sp - 1))
        def _():
            halo_next().wait_send()

        @pl.when(jnp.logical_and(tp == end, sp > 0))
        def _():
            for d in range(1, n_tp):
                halo_side(d).wait_send()

    return start, finish, drain


def project_kernel(n_sp, n_fs, n_tp, *refs):
    tok_ref, gain_ref, wbd_ref = refs[:3]
    w_refs = refs[3:10]
    proj_ref, pre_ref, wo_ref = refs[10:13]
    tokbuf, normbuf, wbuf, loc, tok_s, tok_r, halo_s, halo_r, z_s, z_r, f_s, f_r = refs[13:]
    rows, width = tok_ref.shape
    sp, tp = lax.axis_index("sp"), lax.axis_index("tp")
    count = len(w_refs)
    local = [pltpu.make_async_copy(w_refs[i], wbuf.at[i, sp], loc.at[i]) for i in range(count)]
    here = pltpu.make_async_copy(
        tok_ref, tokbuf.at[pl.ds(pl.multiple_of(halo + tp * rows, 16), rows)], loc.at[count])
    here.start()
    for copy in local:
        copy.start()
    enter(n_sp, n_fs, n_tp)
    start, finish, drain = gather_tokens(n_sp, n_tp, tokbuf, rows, tok_s, tok_r, halo_s, halo_r)
    gather = Gather(n_sp, n_fs, wbuf, z_s, z_r, f_s, f_r)
    here.wait()
    start()
    for w in range(count):
        local[w].wait()
        gather.send(w)
    finish()

    def norm(i, c):
        at = pl.ds(pl.multiple_of(i * 16, 16), 16)
        normbuf[at, :] = rms_rows(tokbuf[at, :], gain_ref[...])
        return c

    lax.fori_loop(0, tokbuf.shape[0] // 16, norm, 0)
    pre_ref[...] = jnp.dot(normbuf[...], wbd_ref[...], preferred_element_type=jnp.float32)
    depth = wbuf.shape[2]

    def project(w):
        total = None
        for s in range(n_sp):
            part = jnp.dot(normbuf[:, s * depth:(s + 1) * depth], wbuf[w, s], preferred_element_type=jnp.float32)
            total = part if total is None else total + part
        proj_ref[w] = total.astype(jnp.bfloat16)

    for w in range(count):
        gather.forward(w)
        if w >= 1:
            gather.finish(w - 1)
            if w - 1 < count - 2:
                project(w - 1)
    gather.flush(count - 1)
    gather.finish(count - 1)
    out = pltpu.make_async_copy(wbuf.at[pl.ds(count - 2, 2)], wo_ref, loc.at[0])
    out.start()
    drain()
    for w in range(count):
        gather.drain(w)
    out.wait()


def project_call(n_sp, n_fs, n_tp, tokens, gain, w_bd, weights):
    rows, width = tokens.shape
    depth, cols = weights[0].shape
    length = halo + n_tp * rows
    count = len(weights)
    slots = max(1, 2 ** len(share_bits(n_fs)) - 1)
    hop = max(1, n_sp - 1)
    dma = pltpu.SemaphoreType.DMA
    vmem, anywhere = pl.BlockSpec(memory_space=pltpu.VMEM), pl.BlockSpec(memory_space=pl.ANY)
    return pl.pallas_call(
        functools.partial(project_kernel, n_sp, n_fs, n_tp),
        out_shape=(
            jax.ShapeDtypeStruct((count - 2, length, cols), jnp.bfloat16),
            jax.ShapeDtypeStruct((length, w_bd.shape[1]), jnp.float32),
            jax.ShapeDtypeStruct((2, n_sp, depth, cols), jnp.bfloat16),
        ),
        in_specs=[anywhere, vmem, vmem] + [anywhere] * count,
        out_specs=(vmem, vmem, anywhere),
        scratch_shapes=[
            pltpu.VMEM((length, width), jnp.bfloat16),
            pltpu.VMEM((length, width), jnp.bfloat16),
            pltpu.VMEM((count, n_sp, depth, cols), jnp.bfloat16),
            dma((count + 1,)), dma((max(1, n_tp - 1),)), dma((max(1, n_tp - 1),)), dma((n_tp,)), dma((n_tp,)),
            dma((count, hop)), dma((count, hop)), dma((count, hop, slots)), dma((count, hop, slots)),
        ],
        compiler_params=pltpu.CompilerParams(collective_id=0, has_side_effects=True, vmem_limit_bytes=50 << 20),
    )(tokens, gain, w_bd, *weights)


def lower_inverse(corr, block):
    at = jnp.arange(block)
    done = jnp.broadcast_to(jnp.eye(block, dtype=jnp.float32), corr.shape)
    size = 1
    while size < block:
        pair = (at[:, None] // (2 * size) == at[None, :] // (2 * size)) & (
            at[:, None] // size != at[None, :] // size)
        off = jnp.where(pair, corr, 0.0)
        if size == 1:
            done = done - off
        else:
            half = jnp.einsum("...ij,...jk->...ik", off, done, precision=highest)
            done = done - jnp.einsum("...ij,...jk->...ik", done, half, precision=highest)
        size *= 2
    return done


def from_behind(block, axis, distance):
    devices = range(lax.axis_size(axis))
    route = [(i - distance, i) for i in devices if i - distance in devices]
    return lax.ppermute(block, axis, route)


def rms_rows(values, gain):
    floats = values.astype(jnp.float32)
    scale = lax.rsqrt(jnp.mean(floats * floats, axis=-1, keepdims=True) + eps)
    return (floats * scale * gain.astype(jnp.float32)).astype(jnp.bfloat16)


def unit_rows(values):
    return values * lax.rsqrt(jnp.sum(values * values, axis=-1, keepdims=True) + eps)


def block_terms(query, keys, values, log_gate, strength, block):
    heads, length, width = keys.shape
    count = length // block

    def split(tensor):
        return tensor.reshape(heads, count, block, tensor.shape[-1])

    query_part, key_part, value_part = (split(query), split(keys), split(values))
    gate_cum = jnp.cumsum(log_gate.reshape(heads, count, block), axis=-1)
    beta_part = strength.reshape(heads, count, block)[..., None]
    lower_mask = jnp.tril(jnp.ones((block, block), dtype=bool))
    strict_mask = jnp.tril(jnp.ones((block, block), dtype=bool), k=-1)
    gaps = gate_cum[..., :, None] - gate_cum[..., None, :]
    decay_tab = jnp.where(lower_mask, jnp.exp(jnp.where(lower_mask, gaps, 0.0)), 0.0)
    key_scaled_beta = key_part * beta_part
    value_beta = value_part * beta_part
    corr_lower = jnp.where(
        strict_mask,
        jnp.einsum("hnid,hnjd->hnij", key_scaled_beta, key_part, precision=highest) * decay_tab,
        0.0,
    )
    inverse = lower_inverse(corr_lower, block)
    fixed_values = jnp.einsum("hnij,hnjd->hnid", inverse, value_beta, precision=highest)
    key_weights = jnp.einsum(
        "hnij,hnjd->hnid",
        inverse,
        key_scaled_beta * jnp.exp(gate_cum)[..., None],
        precision=highest,
    )
    scores = jnp.where(
        lower_mask,
        jnp.einsum("hnid,hnjd->hnij", query_part, key_part, precision=highest) * decay_tab,
        0.0,
    )
    key_decayed = key_part * jnp.exp(gate_cum[..., -1:] - gate_cum)[..., None]
    query_gated = query_part * jnp.exp(gate_cum)[..., None]
    terms = (query_gated, key_decayed, fixed_values, key_weights, scores, gate_cum[..., -1])
    return tuple((jnp.moveaxis(tensor, 1, 0) for tensor in terms))


def carry_step(state, inputs):
    query_gated, key_decayed, fixed_values, key_weights, scores, last_gate = inputs
    fresh = fixed_values - jnp.einsum("hcd,hde->hce", key_weights, state, precision=highest)
    output = jnp.einsum("hcd,hde->hce", query_gated, state, precision=highest) + jnp.einsum(
        "hij,hje->hie", scores, fresh, precision=highest
    )
    state = state * jnp.exp(last_gate)[:, None, None] + jnp.einsum(
        "hcd,hce->hde", key_decayed, fresh, precision=highest
    )
    return (state, output)


def compose_step(carry, inputs):
    linear, offset = carry
    query_gated, key_decayed, fixed_values, key_weights, scores, last_gate = inputs
    fade = jnp.exp(last_gate)[:, None, None]
    moved = jnp.einsum("hcd,hde->hce", key_weights, linear, precision=highest)
    linear = fade * linear - jnp.einsum("hcd,hce->hde", key_decayed, moved, precision=highest)
    fresh = fixed_values - jnp.einsum("hcd,hde->hce", key_weights, offset, precision=highest)
    offset = fade * offset + jnp.einsum("hcd,hce->hde", key_decayed, fresh, precision=highest)
    return ((linear, offset), None)


def apply_map(linear, state):
    return jnp.einsum("hij,hjk->hik", linear, state, precision=highest)


def per_device(
    tokens,
    norm_gain,
    w_pool_in,
    w_query,
    w_key,
    w_value,
    w_gate,
    w_beta,
    w_decay,
    conv_weight,
    a_log,
    decay_extra,
    w_mix,
    pool_scale,
    delta_gain,
    w_out_pool,
    w_out_delta,
):
    n_sp, n_fs, n_tp = (lax.axis_size(a) for a in ("sp", "fs", "tp"))
    proj, both_pre, gathered_out = project_call(
        n_sp, n_fs, n_tp, tokens, norm_gain.reshape(1, -1), jnp.concatenate([w_beta, w_decay], axis=1),
        (w_key, w_query, w_value, w_gate, w_pool_in, w_out_pool, w_out_delta))
    both_pre = both_pre[halo:]
    before = proj[:, halo - tail_rows:halo]
    key_raw, query_raw, value_raw, gate_raw, pool_in = (proj[i, halo:] for i in range(5))
    length = pool_in.shape[0]
    outp_w, outd_w = (
        jnp.transpose(gathered_out[i], (1, 0, 2)).reshape(w_out_pool.shape[0], -1) for i in range(2))
    heads_dev = a_log.shape[0]
    head_dim = query_raw.shape[1] // heads_dev
    width_dev = heads_dev * head_dim
    all_heads = w_beta.shape[1]
    lane = lax.axis_index("tp")
    beta_pre = lax.dynamic_slice_in_dim(both_pre[:, :all_heads], lane * heads_dev, heads_dev, 1)
    forget_logits = lax.dynamic_slice_in_dim(
        both_pre[:, all_heads:], lane * heads_dev, heads_dev, 1
    )
    raw_three = jnp.concatenate([query_raw, key_raw, value_raw], axis=1)
    prior_state = jnp.concatenate([before[4], before[1], before[0], before[2]], axis=1)
    pool_width_dev = pool_in.shape[1]
    source_rows = pool_in.astype(jnp.float32)
    extended = jnp.concatenate(
        [prior_state[:, :pool_width_dev].astype(jnp.float32), source_rows], axis=0
    )
    running = jnp.concatenate(
        [jnp.zeros((1, pool_width_dev), jnp.float32), jnp.cumsum(extended, axis=0)], axis=0
    )
    groups_dev = w_mix.shape[0]
    group_dim = w_mix.shape[1]
    group = lane * groups_dev + jnp.arange(pool_width_dev) // group_dim
    span = (2 ** (1 + group % 4)).astype(jnp.int32)
    ending = running[tail_rows + 1 : tail_rows + 1 + length]
    window_sum = jnp.zeros((length, pool_width_dev), jnp.float32)
    for width in windows:
        lagged = running[tail_rows + 1 - width : tail_rows + 1 - width + length]
        window_sum = window_sum + jnp.where(span[None, :] == width, ending - lagged, 0.0)
    positions = lax.axis_index("sp") * length + jnp.arange(length)
    counts = jnp.minimum(positions[:, None] + 1, span[None, :]).astype(jnp.float32)
    pooled = (window_sum / counts - source_rows).astype(jnp.bfloat16)
    mixed_pool = jnp.einsum(
        "sgc,gcd->sgd",
        pooled.reshape(length, groups_dev, group_dim),
        w_mix,
        preferred_element_type=jnp.float32,
    )
    pool_out = (mixed_pool.reshape(length, pool_width_dev) * pool_scale).astype(jnp.bfloat16)
    taps = conv_weight.shape[1]
    kernel = jnp.transpose(conv_weight, (1, 0, 2)).reshape(taps, 3 * width_dev)
    stacked = jnp.concatenate(
        [prior_state[tail_rows - (taps - 1) :, pool_width_dev:], raw_three], axis=0
    ).astype(jnp.float32)
    conv = jnp.zeros((length, 3 * width_dev), jnp.float32)
    for tap in range(taps):
        conv = conv + stacked[tap : tap + length] * kernel[tap]
    after_silu = jax.nn.silu(conv)

    def heads_first(tensor):
        return jnp.transpose(tensor.reshape(length, heads_dev, head_dim), (1, 0, 2))

    query = unit_rows(heads_first(after_silu[:, :width_dev])) * head_dim ** (-0.5)
    keys = unit_rows(heads_first(after_silu[:, width_dev : 2 * width_dev]))
    values = heads_first(after_silu[:, 2 * width_dev :])
    strength = jax.nn.sigmoid(beta_pre).T
    log_gate = (-jnp.exp(a_log)[None, :] * jax.nn.softplus(forget_logits) + decay_extra).T
    terms = block_terms(query, keys, values, log_gate, strength, BLOCK)
    identity = jnp.broadcast_to(
        jnp.eye(head_dim, dtype=jnp.float32), (heads_dev, head_dim, head_dim)
    )
    empty = jnp.zeros((heads_dev, head_dim, head_dim), jnp.float32)
    (linear, offset), _ = lax.scan(compose_step, (identity, empty), terms)

    def advance(turn, arriving):
        return from_behind(
            (apply_map(linear, arriving) + offset).astype(jnp.bfloat16), "sp", 1
        ).astype(jnp.float32)

    incoming = lax.fori_loop(0, lax.axis_size("sp") - 1, advance, empty)
    _, outputs = lax.scan(carry_step, incoming, terms)
    attended = jnp.transpose(outputs, (1, 0, 2, 3)).reshape(heads_dev, length, head_dim)
    normal_out = (
        attended
        * lax.rsqrt(jnp.mean(attended * attended, axis=-1, keepdims=True) + eps)
        * delta_gain
    )
    gated = normal_out * jax.nn.silu(heads_first(gate_raw.astype(jnp.float32)))
    delta_out = jnp.transpose(gated, (1, 0, 2)).reshape(length, width_dev).astype(jnp.bfloat16)
    value_partial_rows = jnp.dot(pool_out, outp_w, preferred_element_type=jnp.float32) + jnp.dot(
        delta_out, outd_w, preferred_element_type=jnp.float32
    )
    return lax.psum_scatter(
        lax.optimization_barrier(value_partial_rows.astype(jnp.bfloat16))
        .astype(jnp.float32)
        .astype(jnp.bfloat16),
        "tp",
        scatter_dimension=0,
        tiled=True,
    )


def solution(mesh):
    placed = (
        P(("fs", "sp", "tp"), None),
        P(),
        P("sp", "tp"),
        P("sp", "tp"),
        P("sp", "tp"),
        P("sp", "tp"),
        P("sp", "tp"),
        P(),
        P(),
        P(None, None, "tp"),
        P("tp"),
        P(("fs", "sp"), "tp"),
        P("tp", None, None),
        P("tp"),
        P(),
        P("tp", "sp"),
        P("tp", "sp"),
    )
    return jax.shard_map(
        per_device,
        mesh=mesh,
        in_specs=placed,
        out_specs=P(("fs", "sp", "tp"), None),
        check_vma=False,
    )
```

```python
import functools

import jax
import jax.numpy as jnp
from jax import lax
from jax.experimental import pallas as pl
from jax.experimental.pallas import tpu as pltpu
from jax.sharding import PartitionSpec as P

BLOCK = 64
PAIR = 2 * BLOCK

eps = 1e-06
halo = 16
MESH = pl.DeviceIdType.MESH
highest = lax.Precision.HIGHEST
f32 = jnp.float32
bf16 = jnp.bfloat16
KEY, QUERY, VALUE, POOL, GATE, OUT_POOL, OUT_DELTA = range(7)
AHEAD = 1


def mm(a, b, dims=((1,), (0,)), precision=highest):
    return lax.dot_general(a, b, (dims, ((), ())), precision=precision, preferred_element_type=f32)


def rms_rows(values, gain):
    floats = values.astype(f32)
    scale = lax.rsqrt(jnp.mean(floats * floats, axis=-1, keepdims=True) + eps)
    return (floats * scale * gain.astype(f32)).astype(bf16)


def unit_rows(values):
    return values * lax.rsqrt(jnp.sum(values * values, axis=-1, keepdims=True) + eps)


def silu(x):
    return x * jax.nn.sigmoid(x)


def share_bits(n_fs):
    if n_fs & (n_fs - 1):
        return []
    return [n_fs >> (k + 1) for k in range(n_fs.bit_length() - 1)]


class Gather:
    def __init__(self, n_sp, n_fs, wbuf, z_s, z_r, f_s, f_r):
        self.n_sp, self.bits = n_sp, share_bits(n_fs)
        self.wbuf, self.z_s, self.z_r, self.f_s, self.f_r = wbuf, z_s, z_r, f_s, f_r
        self.sp, self.fs = lax.axis_index("sp"), lax.axis_index("fs")
        self.pieces = 2 ** len(self.bits)
        self.mine = self.fs if self.bits else 0 * self.fs
        self.depth = wbuf.shape[2] // self.pieces

    def partner(self, bit):
        return self.fs + bit * (1 - 2 * (self.fs // bit % 2))

    def mask_of(self, m, index):
        for i, bit in enumerate(self.bits):
            if m >> i & 1:
                index = index + bit * (1 - 2 * (index // bit % 2))
        return index

    def piece(self, w, src, index):
        return self.wbuf.at[w, src, pl.ds(pl.multiple_of(index * self.depth, self.depth), self.depth)]

    def z_copy(self, w, src, way):
        ref = self.piece(w, src, self.mine)
        to = lax.rem(self.sp + way + self.n_sp, self.n_sp)
        return pltpu.make_async_remote_copy(
            src_ref=ref, dst_ref=ref, send_sem=self.z_s.at[w, src, (way + 1) // 2], recv_sem=self.z_r.at[w, src],
            device_id={"sp": to}, device_id_type=MESH)

    def f_copy(self, w, src, k, m):
        slot = 2 ** k - 1 + m
        ref = self.piece(w, src, self.mask_of(m, self.mine))
        return pltpu.make_async_remote_copy(
            src_ref=ref, dst_ref=ref, send_sem=self.f_s.at[w, src, slot], recv_sem=self.f_r.at[w, src, slot],
            device_id={"fs": self.partner(self.bits[k])}, device_id_type=MESH)

    def can_send(self, way):
        return self.sp < self.n_sp - 1 if way == 1 else self.sp > 0

    def send(self, w):
        for way in (1, -1):
            @pl.when(self.can_send(way))
            def _():
                self.z_copy(w, self.sp, way).start()

    def each(self, t, act):
        for way in (1, -1):
            src = self.sp - way * t
            @pl.when(src >= 0 if way == 1 else src < self.n_sp)
            def _():
                act(src, way)

    def arrive_z(self, w, src, way):
        self.z_copy(w, src, way).wait_recv()

        @pl.when(self.can_send(way))
        def _():
            self.z_copy(w, src, way).start()
        for k in range(len(self.bits)):
            self.f_copy(w, src, k, 0).start()

    def arrive_f(self, w, t, k):
        def act(src, way):
            for m in range(2 ** k):
                self.f_copy(w, src, k, m).wait_recv()
                for later in range(k + 1, len(self.bits)):
                    self.f_copy(w, src, later, m | 1 << k).start()
        self.each(t, act)

    def forward(self, w):
        last = self.n_sp - 1
        inner = len(self.bits) - 1
        if w + AHEAD < self.wbuf.shape[0]:
            self.send(w + AHEAD)

        def body(t, c):
            self.each(t, lambda src, way: self.arrive_z(w, src, way))
            for k in range(inner):
                @pl.when(t > 1)
                def _():
                    self.arrive_f(w, t - 1, k)
                if w > 0:
                    @pl.when(t == 1)
                    def _():
                        self.arrive_f(w - 1, last, k)
            return c
        lax.fori_loop(1, self.n_sp, body, 0)

    def flush(self, w):
        for k in range(len(self.bits) - 1):
            self.arrive_f(w, self.n_sp - 1, k)

    def finish(self, w):
        if self.bits:
            def body(t, c):
                self.arrive_f(w, t, len(self.bits) - 1)
                return c
            lax.fori_loop(1, self.n_sp, body, 0)

    def drain(self, w):
        for way in (1, -1):
            @pl.when(self.can_send(way))
            def _():
                self.z_copy(w, self.sp, way).wait_send()

        def act(src, way):
            @pl.when(self.can_send(way))
            def _():
                self.z_copy(w, src, way).wait_send()
            for k in range(len(self.bits)):
                for m in range(2 ** k):
                    self.f_copy(w, src, k, m).wait_send()

        def body(t, c):
            self.each(t, act)
            return c
        lax.fori_loop(1, self.n_sp, body, 0)


def enter(n_sp, n_fs, n_tp):
    sp, fs, tp = (lax.axis_index(a) for a in ("sp", "fs", "tp"))
    barrier = pltpu.get_barrier_semaphore()
    bits = share_bits(n_fs)
    for d in range(1, n_sp):
        pl.semaphore_signal(barrier, inc=1, device_id={"sp": lax.rem(sp + d, n_sp)}, device_id_type=MESH)
    for bit in bits:
        pl.semaphore_signal(barrier, inc=1, device_id={"fs": fs + bit * (1 - 2 * (fs // bit % 2))}, device_id_type=MESH)
    for d in range(1, n_tp):
        pl.semaphore_signal(barrier, inc=1, device_id={"tp": lax.rem(tp + d, n_tp)}, device_id_type=MESH)
    pl.semaphore_wait(barrier, n_sp - 1 + len(bits) + n_tp - 1)


def gather_tokens(n_sp, n_tp, tokbuf, rows, tok_s, tok_r, halo_s, halo_r):
    sp, tp = lax.axis_index("sp"), lax.axis_index("tp")

    def tok_copy(d, owner):
        ref = tokbuf.at[pl.ds(pl.multiple_of(halo + owner * rows, 16), rows)]
        return pltpu.make_async_remote_copy(
            src_ref=ref, dst_ref=ref, send_sem=tok_s.at[d - 1], recv_sem=tok_r.at[d - 1],
            device_id={"tp": lax.rem(tp + d, n_tp)}, device_id_type=MESH)

    def halo_next():
        return pltpu.make_async_remote_copy(
            src_ref=tokbuf.at[pl.ds(n_tp * rows, halo)], dst_ref=tokbuf.at[pl.ds(0, halo)],
            send_sem=halo_s.at[0], recv_sem=halo_r.at[0],
            device_id={"sp": lax.rem(sp + 1, n_sp)}, device_id_type=MESH)

    def halo_side(d):
        ref = tokbuf.at[pl.ds(0, halo)]
        return pltpu.make_async_remote_copy(
            src_ref=ref, dst_ref=ref, send_sem=halo_s.at[d], recv_sem=halo_r.at[d],
            device_id={"tp": lax.rem(tp + d, n_tp)}, device_id_type=MESH)

    end = n_tp - 1

    def start():
        for d in range(1, n_tp):
            tok_copy(d, tp).start()

        @pl.when(jnp.logical_and(tp == end, sp < n_sp - 1))
        def _():
            halo_next().start()

        @pl.when(sp == 0)
        def _():
            tokbuf[0:halo, :] = jnp.zeros((halo, tokbuf.shape[1]), tokbuf.dtype)

    def finish():
        @pl.when(jnp.logical_and(tp == end, sp > 0))
        def _():
            halo_next().wait_recv()
            for d in range(1, n_tp):
                halo_side(d).start()
        for d in range(1, n_tp):
            tok_copy(d, lax.rem(tp - d + n_tp, n_tp)).wait_recv()

        @pl.when(jnp.logical_and(tp < end, sp > 0))
        def _():
            for d in range(1, n_tp):
                @pl.when(tp == d - 1)
                def _():
                    halo_side(d).wait_recv()

    def drain():
        for d in range(1, n_tp):
            tok_copy(d, tp).wait_send()

        @pl.when(jnp.logical_and(tp == end, sp < n_sp - 1))
        def _():
            halo_next().wait_send()

        @pl.when(jnp.logical_and(tp == end, sp > 0))
        def _():
            for d in range(1, n_tp):
                halo_side(d).wait_send()

    return start, finish, drain


def mixer_kernel(n_sp, n_fs, n_tp, *refs):
    tok_ref, gain_ref, wbd_ref, conv_ref, alog_ref, extra_ref, mix_ref, scale_ref, dgain_ref = refs[:9]
    w_refs = refs[9:16]
    out_ref = refs[16]
    (tokbuf, normbuf, wbuf, raw, pool_out, delta_out, pbuf, cbuf, s_in, s_out, part, rsbuf,
     loc, tok_s, tok_r, halo_s, halo_r, z_s, z_r, f_s, f_r, st_s, st_r, rs_s, rs_r) = refs[17:]
    rows, width = tok_ref.shape
    length = n_tp * rows
    heads, head_dim = cbuf.shape[0], cbuf.shape[1]
    groups, group_dim = mix_ref.shape[0], mix_ref.shape[1]
    sp, tp = lax.axis_index("sp"), lax.axis_index("tp")
    count = len(w_refs)
    local = [pltpu.make_async_copy(w_refs[i], wbuf.at[i, sp], loc.at[i]) for i in range(count)]
    here = pltpu.make_async_copy(
        tok_ref, tokbuf.at[pl.ds(pl.multiple_of(halo + tp * rows, 16), rows)], loc.at[count])
    here.start()
    for copy in local:
        copy.start()
    enter(n_sp, n_fs, n_tp)
    start, finish, drain = gather_tokens(n_sp, n_tp, tokbuf, rows, tok_s, tok_r, halo_s, halo_r)
    gather = Gather(n_sp, n_fs, wbuf, z_s, z_r, f_s, f_r)
    here.wait()
    start()
    for w in range(count):
        local[w].wait()
        if w < AHEAD:
            gather.send(w)
    depth = wbuf.shape[2]

    def norm(i, c):
        at = pl.ds(pl.multiple_of(i * 16, 16), 16)
        normbuf[at, :] = rms_rows(tokbuf[at, :], gain_ref[...])
        return c

    def project(w):
        total = None
        for s in range(n_sp):
            term = jnp.dot(normbuf[:, s * depth:(s + 1) * depth], wbuf[w, s], preferred_element_type=f32)
            total = term if total is None else total + term
        raw[w] = total.astype(bf16).astype(f32)

    gather.forward(0)
    finish()
    lax.fori_loop(0, tokbuf.shape[0] // 16, norm, 0)
    pre = jnp.dot(normbuf[...], wbd_ref[...], preferred_element_type=f32)[halo:]
    softplus = jnp.maximum(pre, 0.0) + jnp.log1p(jnp.exp(-jnp.abs(pre)))
    log_gate = -jnp.exp(alog_ref[...]) * softplus + extra_ref[...]
    strength = jax.nn.sigmoid(pre)
    row = lax.broadcasted_iota(jnp.int32, (length, length), 0)
    col = lax.broadcasted_iota(jnp.int32, (length, length), 1)
    tri = jnp.where((row // BLOCK == col // BLOCK) & (row >= col), 1.0, 0.0)
    cum = mm(tri, log_gate)
    cum_t = cum.T

    gather.forward(1)
    gather.finish(0)
    project(0)
    gather.forward(2)
    gather.finish(1)
    project(1)
    gather.forward(3)
    gather.finish(2)
    project(2)

    def active(role, w, h):
        at = slice(h * head_dim, (h + 1) * head_dim)
        taps = conv_ref.shape[1]
        total = None
        for j in range(taps):
            term = raw[w, pl.ds(halo - (taps - 1) + j, length), at] * conv_ref[role, j:j + 1, at]
            total = term if total is None else total + term
        return silu(total)

    unit = min(PAIR, length)
    i2 = lax.broadcasted_iota(jnp.int32, (unit, unit), 0)
    j2 = lax.broadcasted_iota(jnp.int32, (unit, unit), 1)
    lower = (i2 // BLOCK == j2 // BLOCK) & (i2 >= j2)
    strict = lower & (i2 > j2)
    eye = jnp.where(i2 == j2, 1.0, 0.0)

    def delta(some):
        units = []
        for h in some:
            q = unit_rows(active(0, QUERY, h)) * head_dim ** (-0.5)
            k = unit_rows(active(1, KEY, h))
            v = active(2, VALUE, h)
            beta = strength[:, heads + h:heads + h + 1]
            g = cum[:, h:h + 1]
            grow = jnp.exp(g)
            kb = k * beta
            right = jnp.concatenate([v * beta, kb * grow], axis=1)
            qg = q * grow
            for p in range(length // unit):
                at = slice(p * unit, (p + 1) * unit)
                gaps = g[at] - cum_t[h:h + 1, at]
                decay = jnp.where(lower, jnp.exp(jnp.where(lower, gaps, 0.0)), 0.0)
                both = mm(jnp.concatenate([kb[at], q[at]], axis=0), k[at], ((1,), (1,)))
                corr = jnp.where(strict, both[:unit] * decay, 0.0)
                scores = both[unit:] * decay
                units.append([h, p, corr, scores, right[at], qg[at], k[at], g[at]])
        done = [eye - jnp.where((i2 // 2 == j2 // 2), u[2], 0.0) for u in units]
        size = 2
        while size < BLOCK:
            pair = (i2 // (2 * size) == j2 // (2 * size)) & (i2 // size != j2 // size)
            half = [mm(jnp.where(pair, u[2], 0.0), x) for u, x in zip(units, done)]
            done = [x - mm(x, y) for x, y in zip(done, half)]
            size *= 2
        solved = [mm(x, u[4]) for u, x in zip(units, done)]
        carry = {h: jnp.concatenate([jnp.where(
            lax.broadcasted_iota(jnp.int32, (head_dim, head_dim), 0)
            == lax.broadcasted_iota(jnp.int32, (head_dim, head_dim), 1), 1.0, 0.0),
            jnp.zeros((head_dim, head_dim), f32)], axis=1) for h in some}
        per = length // unit
        for p in range(per):
            for b in range(unit // BLOCK):
                at = slice(b * BLOCK, (b + 1) * BLOCK)
                for n, h in enumerate(some):
                    _, _, _, scores, _, qg, k, g = units[n * per + p]
                    fixed = solved[n * per + p][at, :head_dim]
                    kw = solved[n * per + p][at, head_dim:]
                    last = g[(b + 1) * BLOCK - 1:(b + 1) * BLOCK]
                    fall = k[at] * jnp.exp(last - g[at])
                    c = carry[h]
                    two = mm(jnp.concatenate([kw, qg[at]], axis=0), c)
                    fresh = jnp.concatenate([jnp.zeros_like(fixed), fixed], axis=1) - two[:BLOCK]
                    pbuf[h, p * unit + b * BLOCK:p * unit + (b + 1) * BLOCK, :] = (
                        two[BLOCK:] + mm(scores[at, at], fresh))
                    carry[h] = jnp.exp(last) * c + mm(fall, fresh, ((0,), (0,)))
        for h in some:
            cbuf[h] = carry[h]

    def pool():
        at_row = lax.broadcasted_iota(jnp.int32, (length, group_dim), 0) + sp * length
        for i in range(groups):
            at = slice(i * group_dim, (i + 1) * group_dim)
            x = raw[POOL, :, at]
            span = 2 * jnp.left_shift(1, lax.rem(tp * groups + i, 4))
            total = x
            window = jnp.zeros_like(x)
            for w in (2, 4, 8, 16):
                total = total + pltpu.roll(total, w // 2, 0)
                window = window + jnp.where(span == w, total, 0.0)
            tally = jnp.minimum(at_row + 1, span).astype(f32)
            pooled = (window[halo:] / tally - x[halo:]).astype(bf16)
            mixed = jnp.dot(pooled, mix_ref[i], preferred_element_type=f32)
            pool_out[:, at] = (mixed * scale_ref[:, at]).astype(bf16)

    cut = (heads + 1) // 2
    delta(range(cut))
    gather.forward(4)
    gather.finish(3)
    project(3)
    if cut < heads:
        delta(range(cut, heads))
    gather.forward(5)
    gather.finish(4)
    project(4)

    def state_copy(h):
        return pltpu.make_async_remote_copy(
            src_ref=s_out.at[h], dst_ref=s_in.at[h], send_sem=st_s.at[h], recv_sem=st_r.at[h],
            device_id={"sp": lax.rem(sp + 1, n_sp)}, device_id_type=MESH)

    @pl.when(sp == 0)
    def _():
        s_in[...] = jnp.zeros_like(s_in)

    gather.forward(6)
    gather.finish(5)
    pool()
    for h in range(heads):
        @pl.when(sp > 0)
        def _():
            state_copy(h).wait_recv()
        s_out[h] = (mm(cbuf[h, :, :head_dim], s_in[h].astype(f32)) + cbuf[h, :, head_dim:]).astype(bf16)

        @pl.when(sp < n_sp - 1)
        def _():
            state_copy(h).start()
    gather.flush(6)
    for h in range(heads):
        at = slice(h * head_dim, (h + 1) * head_dim)
        attended = mm(pbuf[h, :, :head_dim], s_in[h].astype(f32)) + pbuf[h, :, head_dim:]
        scale = lax.rsqrt(jnp.mean(attended * attended, axis=-1, keepdims=True) + eps)
        delta_out[:, at] = (attended * scale * dgain_ref[...] * silu(raw[GATE, halo:, at])).astype(bf16)
    gather.finish(6)

    def rs_copy(s, d, owner, dest):
        return pltpu.make_async_remote_copy(
            src_ref=part.at[s, pl.ds(pl.multiple_of(dest * rows, 16), rows)], dst_ref=rsbuf.at[s, owner],
            send_sem=rs_s.at[s, d - 1], recv_sem=rs_r.at[s, d - 1],
            device_id={"tp": lax.rem(tp + d, n_tp)}, device_id_type=MESH)

    for s in range(n_sp):
        part[s] = (jnp.dot(pool_out[...], wbuf[OUT_POOL, s], preferred_element_type=f32)
                   + jnp.dot(delta_out[...], wbuf[OUT_DELTA, s], preferred_element_type=f32)).astype(bf16)
        for d in range(1, n_tp):
            rs_copy(s, d, tp, lax.rem(tp + d, n_tp)).start()
    cols = wbuf.shape[3]
    for s in range(n_sp):
        total = part[s, pl.ds(pl.multiple_of(tp * rows, 16), rows)].astype(f32)
        for d in range(1, n_tp):
            owner = lax.rem(tp - d + n_tp, n_tp)
            rs_copy(s, d, owner, tp).wait_recv()
            total = total + rsbuf[s, owner].astype(f32)
        out_ref[:, s * cols:(s + 1) * cols] = total.astype(bf16)
    drain()
    for w in range(count):
        gather.drain(w)

    @pl.when(sp < n_sp - 1)
    def _():
        for h in range(heads):
            state_copy(h).wait_send()
    for s in range(n_sp):
        for d in range(1, n_tp):
            rs_copy(s, d, tp, lax.rem(tp + d, n_tp)).wait_send()


def per_device(
    tokens,
    norm_gain,
    w_pool_in,
    w_query,
    w_key,
    w_value,
    w_gate,
    w_beta,
    w_decay,
    conv_weight,
    a_log,
    decay_extra,
    w_mix,
    pool_scale,
    delta_gain,
    w_out_pool,
    w_out_delta,
):
    n_sp, n_fs, n_tp = (lax.axis_size(a) for a in ("sp", "fs", "tp"))
    weights = (w_key, w_query, w_value, w_pool_in, w_gate, w_out_pool, w_out_delta)
    rows, width = tokens.shape
    depth, cols = w_key.shape
    heads = a_log.shape[0]
    head_dim = cols // heads
    length = n_tp * rows
    count = len(weights)
    lanes = 128
    lane = lax.axis_index("tp")

    def own(w):
        return lax.dynamic_slice_in_dim(w, lane * heads, heads, 1)

    def wide(x):
        return jnp.pad(x, ((0, 0), (0, lanes - x.shape[1])))

    w_bd = wide(jnp.concatenate([own(w_decay), own(w_beta)], axis=1))
    slots = max(1, 2 ** len(share_bits(n_fs)) - 1)
    side = max(1, n_tp - 1)
    dma = pltpu.SemaphoreType.DMA
    vmem, anywhere = pl.BlockSpec(memory_space=pltpu.VMEM), pl.BlockSpec(memory_space=pl.ANY)
    return pl.pallas_call(
        functools.partial(mixer_kernel, n_sp, n_fs, n_tp),
        out_shape=jax.ShapeDtypeStruct((rows, width), bf16),
        in_specs=[anywhere] + [vmem] * 8 + [anywhere] * count,
        out_specs=vmem,
        scratch_shapes=[
            pltpu.VMEM((halo + length, width), bf16),
            pltpu.VMEM((halo + length, width), bf16),
            pltpu.VMEM((count, n_sp, depth, cols), bf16),
            pltpu.VMEM((5, halo + length, cols), f32),
            pltpu.VMEM((length, cols), bf16),
            pltpu.VMEM((length, cols), bf16),
            pltpu.VMEM((heads, length, 2 * head_dim), f32),
            pltpu.VMEM((heads, head_dim, 2 * head_dim), f32),
            pltpu.VMEM((heads, head_dim, head_dim), bf16),
            pltpu.VMEM((heads, head_dim, head_dim), bf16),
            pltpu.VMEM((n_sp, length, cols), bf16),
            pltpu.VMEM((n_sp, n_tp, rows, cols), bf16),
            dma((count + 1,)), dma((side,)), dma((side,)), dma((n_tp,)), dma((n_tp,)),
            dma((count, n_sp, 2)), dma((count, n_sp)), dma((count, n_sp, slots)), dma((count, n_sp, slots)),
            dma((heads,)), dma((heads,)), dma((n_sp, side)), dma((n_sp, side)),
        ],
        compiler_params=pltpu.CompilerParams(collective_id=0, has_side_effects=True, vmem_limit_bytes=56 << 20),
    )(tokens, norm_gain.reshape(1, -1), w_bd, conv_weight, wide(a_log.reshape(1, -1)), wide(decay_extra), w_mix,
      pool_scale.reshape(1, -1), delta_gain.reshape(1, -1), *weights)


def solution(mesh):
    placed = (
        P(("fs", "sp", "tp"), None),
        P(),
        P("sp", "tp"),
        P("sp", "tp"),
        P("sp", "tp"),
        P("sp", "tp"),
        P("sp", "tp"),
        P(),
        P(),
        P(None, None, "tp"),
        P("tp"),
        P(("fs", "sp"), "tp"),
        P("tp", None, None),
        P("tp"),
        P(),
        P("tp", "sp"),
        P("tp", "sp"),
    )
    return jax.shard_map(
        per_device,
        mesh=mesh,
        in_specs=placed,
        out_specs=P(("fs", "sp", "tp"), None),
        check_vma=False,
    )
```

```python
import functools

import jax
import jax.numpy as jnp
from jax import lax
from jax.experimental import pallas as pl
from jax.experimental.pallas import tpu as pltpu
from jax.sharding import PartitionSpec as P

BLOCK = 64
PAIR = 2 * BLOCK

eps = 1e-06
halo = 16
MESH = pl.DeviceIdType.MESH
highest = lax.Precision.HIGHEST
f32 = jnp.float32
bf16 = jnp.bfloat16
KEY, QUERY, VALUE, POOL, GATE, OUT_POOL, OUT_DELTA = range(7)
AHEAD = 1


def mm(a, b, dims=((1,), (0,)), precision=highest):
    return lax.dot_general(a, b, (dims, ((), ())), precision=precision, preferred_element_type=f32)


def rms_rows(values, gain):
    floats = values.astype(f32)
    scale = lax.rsqrt(jnp.mean(floats * floats, axis=-1, keepdims=True) + eps)
    return (floats * scale * gain.astype(f32)).astype(bf16)


def unit_rows(values):
    return values * lax.rsqrt(jnp.sum(values * values, axis=-1, keepdims=True) + eps)


def silu(x):
    return x * jax.nn.sigmoid(x)


def share_bits(n_fs):
    if n_fs & (n_fs - 1):
        return []
    return [n_fs >> (k + 1) for k in range(n_fs.bit_length() - 1)]


class Gather:
    def __init__(self, n_sp, n_fs, wbuf, z_s, z_r, f_s, f_r):
        self.n_sp, self.bits = n_sp, share_bits(n_fs)
        self.wbuf, self.z_s, self.z_r, self.f_s, self.f_r = wbuf, z_s, z_r, f_s, f_r
        self.sp, self.fs = lax.axis_index("sp"), lax.axis_index("fs")
        self.pieces = 2 ** len(self.bits)
        self.mine = self.fs if self.bits else 0 * self.fs
        self.depth = wbuf.shape[2] // self.pieces

    def partner(self, bit):
        return self.fs + bit * (1 - 2 * (self.fs // bit % 2))

    def mask_of(self, m, index):
        for i, bit in enumerate(self.bits):
            if m >> i & 1:
                index = index + bit * (1 - 2 * (index // bit % 2))
        return index

    def piece(self, w, src, index):
        return self.wbuf.at[w, src, pl.ds(pl.multiple_of(index * self.depth, self.depth), self.depth)]

    def z_copy(self, w, src, way):
        ref = self.piece(w, src, self.mine)
        to = lax.rem(self.sp + way + self.n_sp, self.n_sp)
        return pltpu.make_async_remote_copy(
            src_ref=ref, dst_ref=ref, send_sem=self.z_s.at[w, src, (way + 1) // 2], recv_sem=self.z_r.at[w, src],
            device_id={"sp": to}, device_id_type=MESH)

    def f_copy(self, w, src, k, m):
        slot = 2 ** k - 1 + m
        ref = self.piece(w, src, self.mask_of(m, self.mine))
        return pltpu.make_async_remote_copy(
            src_ref=ref, dst_ref=ref, send_sem=self.f_s.at[w, src, slot], recv_sem=self.f_r.at[w, src, slot],
            device_id={"fs": self.partner(self.bits[k])}, device_id_type=MESH)

    def can_send(self, way):
        return self.sp < self.n_sp - 1 if way == 1 else self.sp > 0

    def send(self, w):
        for way in (1, -1):
            @pl.when(self.can_send(way))
            def _():
                self.z_copy(w, self.sp, way).start()

    def each(self, t, act):
        for way in (1, -1):
            src = self.sp - way * t
            @pl.when(src >= 0 if way == 1 else src < self.n_sp)
            def _():
                act(src, way)

    def arrive_z(self, w, src, way):
        self.z_copy(w, src, way).wait_recv()

        @pl.when(self.can_send(way))
        def _():
            self.z_copy(w, src, way).start()
        for k in range(len(self.bits)):
            self.f_copy(w, src, k, 0).start()

    def arrive_f(self, w, t, k):
        def act(src, way):
            for m in range(2 ** k):
                self.f_copy(w, src, k, m).wait_recv()
                for later in range(k + 1, len(self.bits)):
                    self.f_copy(w, src, later, m | 1 << k).start()
        self.each(t, act)

    def forward(self, w):
        last = self.n_sp - 1
        inner = len(self.bits) - 1
        if w + AHEAD < self.wbuf.shape[0]:
            self.send(w + AHEAD)

        def body(t, c):
            self.each(t, lambda src, way: self.arrive_z(w, src, way))
            for k in range(inner):
                @pl.when(t > 1)
                def _():
                    self.arrive_f(w, t - 1, k)
                if w > 0:
                    @pl.when(t == 1)
                    def _():
                        self.arrive_f(w - 1, last, k)
            return c
        lax.fori_loop(1, self.n_sp, body, 0)

    def flush(self, w):
        for k in range(len(self.bits) - 1):
            self.arrive_f(w, self.n_sp - 1, k)

    def finish(self, w):
        if self.bits:
            def body(t, c):
                self.arrive_f(w, t, len(self.bits) - 1)
                return c
            lax.fori_loop(1, self.n_sp, body, 0)

    def drain(self, w):
        for way in (1, -1):
            @pl.when(self.can_send(way))
            def _():
                self.z_copy(w, self.sp, way).wait_send()

        def act(src, way):
            @pl.when(self.can_send(way))
            def _():
                self.z_copy(w, src, way).wait_send()
            for k in range(len(self.bits)):
                for m in range(2 ** k):
                    self.f_copy(w, src, k, m).wait_send()

        def body(t, c):
            self.each(t, act)
            return c
        lax.fori_loop(1, self.n_sp, body, 0)


def enter(n_sp, n_fs, n_tp):
    sp, fs, tp = (lax.axis_index(a) for a in ("sp", "fs", "tp"))
    barrier = pltpu.get_barrier_semaphore()
    bits = share_bits(n_fs)
    for d in range(1, n_sp):
        pl.semaphore_signal(barrier, inc=1, device_id={"sp": lax.rem(sp + d, n_sp)}, device_id_type=MESH)
    for bit in bits:
        pl.semaphore_signal(barrier, inc=1, device_id={"fs": fs + bit * (1 - 2 * (fs // bit % 2))}, device_id_type=MESH)
    for d in range(1, n_tp):
        pl.semaphore_signal(barrier, inc=1, device_id={"tp": lax.rem(tp + d, n_tp)}, device_id_type=MESH)
    pl.semaphore_wait(barrier, n_sp - 1 + len(bits) + n_tp - 1)


def gather_tokens(n_sp, n_tp, tokbuf, rows, tok_s, tok_r, halo_s, halo_r):
    sp, tp = lax.axis_index("sp"), lax.axis_index("tp")

    def tok_copy(d, owner):
        ref = tokbuf.at[pl.ds(pl.multiple_of(halo + owner * rows, 16), rows)]
        return pltpu.make_async_remote_copy(
            src_ref=ref, dst_ref=ref, send_sem=tok_s.at[d - 1], recv_sem=tok_r.at[d - 1],
            device_id={"tp": lax.rem(tp + d, n_tp)}, device_id_type=MESH)

    def halo_next():
        return pltpu.make_async_remote_copy(
            src_ref=tokbuf.at[pl.ds(n_tp * rows, halo)], dst_ref=tokbuf.at[pl.ds(0, halo)],
            send_sem=halo_s.at[0], recv_sem=halo_r.at[0],
            device_id={"sp": lax.rem(sp + 1, n_sp)}, device_id_type=MESH)

    def halo_side(d):
        ref = tokbuf.at[pl.ds(0, halo)]
        return pltpu.make_async_remote_copy(
            src_ref=ref, dst_ref=ref, send_sem=halo_s.at[d], recv_sem=halo_r.at[d],
            device_id={"tp": lax.rem(tp + d, n_tp)}, device_id_type=MESH)

    end = n_tp - 1

    def start():
        for d in range(1, n_tp):
            tok_copy(d, tp).start()

        @pl.when(jnp.logical_and(tp == end, sp < n_sp - 1))
        def _():
            halo_next().start()

        @pl.when(sp == 0)
        def _():
            tokbuf[0:halo, :] = jnp.zeros((halo, tokbuf.shape[1]), tokbuf.dtype)

    def finish():
        @pl.when(jnp.logical_and(tp == end, sp > 0))
        def _():
            halo_next().wait_recv()
            for d in range(1, n_tp):
                halo_side(d).start()
        for d in range(1, n_tp):
            tok_copy(d, lax.rem(tp - d + n_tp, n_tp)).wait_recv()

        @pl.when(jnp.logical_and(tp < end, sp > 0))
        def _():
            for d in range(1, n_tp):
                @pl.when(tp == d - 1)
                def _():
                    halo_side(d).wait_recv()

    def drain():
        for d in range(1, n_tp):
            tok_copy(d, tp).wait_send()

        @pl.when(jnp.logical_and(tp == end, sp < n_sp - 1))
        def _():
            halo_next().wait_send()

        @pl.when(jnp.logical_and(tp == end, sp > 0))
        def _():
            for d in range(1, n_tp):
                halo_side(d).wait_send()

    return start, finish, drain


def mixer_kernel(n_sp, n_fs, n_tp, *refs):
    tok_ref, gain_ref, wbd_ref, conv_ref, alog_ref, extra_ref, mix_ref, scale_ref, dgain_ref = refs[:9]
    w_refs = refs[9:16]
    out_ref = refs[16]
    (tokbuf, normbuf, wbuf, raw, pool_out, delta_out, pbuf, cbuf, s_in, s_out, part, rsbuf,
     loc, tok_s, tok_r, halo_s, halo_r, z_s, z_r, f_s, f_r, st_s, st_r, rs_s, rs_r) = refs[17:]
    rows, width = tok_ref.shape
    length = n_tp * rows
    heads, head_dim = cbuf.shape[0], cbuf.shape[1]
    groups, group_dim = mix_ref.shape[0], mix_ref.shape[1]
    sp, tp = lax.axis_index("sp"), lax.axis_index("tp")
    count = len(w_refs)
    local = [pltpu.make_async_copy(w_refs[i], wbuf.at[i, sp], loc.at[i]) for i in range(count)]
    here = pltpu.make_async_copy(
        tok_ref, tokbuf.at[pl.ds(pl.multiple_of(halo + tp * rows, 16), rows)], loc.at[count])
    here.start()
    for copy in local:
        copy.start()
    enter(n_sp, n_fs, n_tp)
    start, finish, drain = gather_tokens(n_sp, n_tp, tokbuf, rows, tok_s, tok_r, halo_s, halo_r)
    gather = Gather(n_sp, n_fs, wbuf, z_s, z_r, f_s, f_r)
    here.wait()
    start()
    for w in range(count):
        local[w].wait()
        if w < AHEAD:
            gather.send(w)
    depth = wbuf.shape[2]

    def norm(i, c):
        at = pl.ds(pl.multiple_of(i * 16, 16), 16)
        normbuf[at, :] = rms_rows(tokbuf[at, :], gain_ref[...])
        return c

    def project(w):
        total = None
        for s in range(n_sp):
            term = jnp.dot(normbuf[:, s * depth:(s + 1) * depth], wbuf[w, s], preferred_element_type=f32)
            total = term if total is None else total + term
        raw[w] = total.astype(bf16).astype(f32)

    gather.forward(0)
    gather.forward(1)
    finish()
    lax.fori_loop(0, tokbuf.shape[0] // 16, norm, 0)
    pre = jnp.dot(normbuf[...], wbd_ref[...], preferred_element_type=f32)[halo:]
    softplus = jnp.maximum(pre, 0.0) + jnp.log1p(jnp.exp(-jnp.abs(pre)))
    log_gate = -jnp.exp(alog_ref[...]) * softplus + extra_ref[...]
    strength = jax.nn.sigmoid(pre)
    row = lax.broadcasted_iota(jnp.int32, (length, length), 0)
    col = lax.broadcasted_iota(jnp.int32, (length, length), 1)
    tri = jnp.where((row // BLOCK == col // BLOCK) & (row >= col), 1.0, 0.0)
    cum = mm(tri, log_gate)
    cum_t = cum.T

    gather.finish(0)
    project(0)
    gather.forward(2)
    gather.finish(1)
    project(1)
    gather.forward(3)
    gather.finish(2)
    project(2)

    def active(role, w, h):
        at = slice(h * head_dim, (h + 1) * head_dim)
        taps = conv_ref.shape[1]
        total = None
        for j in range(taps):
            term = raw[w, pl.ds(halo - (taps - 1) + j, length), at] * conv_ref[role, j:j + 1, at]
            total = term if total is None else total + term
        return silu(total)

    unit = min(PAIR, length)
    i2 = lax.broadcasted_iota(jnp.int32, (unit, unit), 0)
    j2 = lax.broadcasted_iota(jnp.int32, (unit, unit), 1)
    lower = (i2 // BLOCK == j2 // BLOCK) & (i2 >= j2)
    strict = lower & (i2 > j2)
    eye = jnp.where(i2 == j2, 1.0, 0.0)

    def delta(some):
        units = []
        for h in some:
            q = unit_rows(active(0, QUERY, h)) * head_dim ** (-0.5)
            k = unit_rows(active(1, KEY, h))
            v = active(2, VALUE, h)
            beta = strength[:, heads + h:heads + h + 1]
            g = cum[:, h:h + 1]
            grow = jnp.exp(g)
            kb = k * beta
            right = jnp.concatenate([v * beta, kb * grow], axis=1)
            qg = q * grow
            for p in range(length // unit):
                at = slice(p * unit, (p + 1) * unit)
                gaps = g[at] - cum_t[h:h + 1, at]
                decay = jnp.where(lower, jnp.exp(jnp.where(lower, gaps, 0.0)), 0.0)
                both = mm(jnp.concatenate([kb[at], q[at]], axis=0), k[at], ((1,), (1,)))
                corr = jnp.where(strict, both[:unit] * decay, 0.0)
                scores = both[unit:] * decay
                units.append([h, p, corr, scores, right[at], qg[at], k[at], g[at]])
        done = [eye - jnp.where((i2 // 2 == j2 // 2), u[2], 0.0) for u in units]
        size = 2
        while size < BLOCK:
            pair = (i2 // (2 * size) == j2 // (2 * size)) & (i2 // size != j2 // size)
            half = [mm(jnp.where(pair, u[2], 0.0), x) for u, x in zip(units, done)]
            done = [x - mm(x, y) for x, y in zip(done, half)]
            size *= 2
        solved = [mm(x, u[4]) for u, x in zip(units, done)]
        carry = {h: jnp.concatenate([jnp.where(
            lax.broadcasted_iota(jnp.int32, (head_dim, head_dim), 0)
            == lax.broadcasted_iota(jnp.int32, (head_dim, head_dim), 1), 1.0, 0.0),
            jnp.zeros((head_dim, head_dim), f32)], axis=1) for h in some}
        per = length // unit
        for p in range(per):
            for b in range(unit // BLOCK):
                at = slice(b * BLOCK, (b + 1) * BLOCK)
                for n, h in enumerate(some):
                    _, _, _, scores, _, qg, k, g = units[n * per + p]
                    fixed = solved[n * per + p][at, :head_dim]
                    kw = solved[n * per + p][at, head_dim:]
                    last = g[(b + 1) * BLOCK - 1:(b + 1) * BLOCK]
                    fall = k[at] * jnp.exp(last - g[at])
                    c = carry[h]
                    two = mm(jnp.concatenate([kw, qg[at]], axis=0), c, precision=None)
                    fresh = jnp.concatenate([jnp.zeros_like(fixed), fixed], axis=1) - two[:BLOCK]
                    pbuf[h, p * unit + b * BLOCK:p * unit + (b + 1) * BLOCK, :] = (
                        two[BLOCK:] + mm(scores[at, at], fresh, precision=None))
                    carry[h] = jnp.exp(last) * c + mm(fall, fresh, ((0,), (0,)), None)
        for h in some:
            cbuf[h] = carry[h]

    def pool():
        at_row = lax.broadcasted_iota(jnp.int32, (length, group_dim), 0) + sp * length
        for i in range(groups):
            at = slice(i * group_dim, (i + 1) * group_dim)
            x = raw[POOL, :, at]
            span = 2 * jnp.left_shift(1, lax.rem(tp * groups + i, 4))
            total = x
            window = jnp.zeros_like(x)
            for w in (2, 4, 8, 16):
                total = total + pltpu.roll(total, w // 2, 0)
                window = window + jnp.where(span == w, total, 0.0)
            tally = jnp.minimum(at_row + 1, span).astype(f32)
            pooled = (window[halo:] / tally - x[halo:]).astype(bf16)
            mixed = jnp.dot(pooled, mix_ref[i], preferred_element_type=f32)
            pool_out[:, at] = (mixed * scale_ref[:, at]).astype(bf16)

    cut = (heads + 1) // 2
    delta(range(cut))
    gather.forward(4)
    gather.finish(3)
    project(3)
    if cut < heads:
        delta(range(cut, heads))
    gather.forward(5)
    gather.finish(4)
    project(4)

    def state_copy(h):
        return pltpu.make_async_remote_copy(
            src_ref=s_out.at[h], dst_ref=s_in.at[h], send_sem=st_s.at[h], recv_sem=st_r.at[h],
            device_id={"sp": lax.rem(sp + 1, n_sp)}, device_id_type=MESH)

    @pl.when(sp == 0)
    def _():
        s_in[...] = jnp.zeros_like(s_in)

    gather.forward(6)
    gather.finish(5)
    pool()
    for h in range(heads):
        @pl.when(sp > 0)
        def _():
            state_copy(h).wait_recv()
        s_out[h] = (mm(cbuf[h, :, :head_dim], s_in[h].astype(f32), precision=None) + cbuf[h, :, head_dim:]).astype(bf16)

        @pl.when(sp < n_sp - 1)
        def _():
            state_copy(h).start()
    gather.flush(6)
    for h in range(heads):
        at = slice(h * head_dim, (h + 1) * head_dim)
        attended = mm(pbuf[h, :, :head_dim], s_in[h].astype(f32), precision=None) + pbuf[h, :, head_dim:]
        scale = lax.rsqrt(jnp.mean(attended * attended, axis=-1, keepdims=True) + eps)
        delta_out[:, at] = (attended * scale * dgain_ref[...] * silu(raw[GATE, halo:, at])).astype(bf16)
    gather.finish(6)

    def rs_copy(s, d, owner, dest):
        return pltpu.make_async_remote_copy(
            src_ref=part.at[s, pl.ds(pl.multiple_of(dest * rows, 16), rows)], dst_ref=rsbuf.at[s, owner],
            send_sem=rs_s.at[s, d - 1], recv_sem=rs_r.at[s, d - 1],
            device_id={"tp": lax.rem(tp + d, n_tp)}, device_id_type=MESH)

    for s in range(n_sp):
        part[s] = (jnp.dot(pool_out[...], wbuf[OUT_POOL, s], preferred_element_type=f32)
                   + jnp.dot(delta_out[...], wbuf[OUT_DELTA, s], preferred_element_type=f32)).astype(bf16)
        for d in range(1, n_tp):
            rs_copy(s, d, tp, lax.rem(tp + d, n_tp)).start()
    cols = wbuf.shape[3]
    for s in range(n_sp):
        total = part[s, pl.ds(pl.multiple_of(tp * rows, 16), rows)].astype(f32)
        for d in range(1, n_tp):
            owner = lax.rem(tp - d + n_tp, n_tp)
            rs_copy(s, d, owner, tp).wait_recv()
            total = total + rsbuf[s, owner].astype(f32)
        out_ref[:, s * cols:(s + 1) * cols] = total.astype(bf16)
    drain()
    for w in range(count):
        gather.drain(w)

    @pl.when(sp < n_sp - 1)
    def _():
        for h in range(heads):
            state_copy(h).wait_send()
    for s in range(n_sp):
        for d in range(1, n_tp):
            rs_copy(s, d, tp, lax.rem(tp + d, n_tp)).wait_send()


def per_device(
    tokens,
    norm_gain,
    w_pool_in,
    w_query,
    w_key,
    w_value,
    w_gate,
    w_beta,
    w_decay,
    conv_weight,
    a_log,
    decay_extra,
    w_mix,
    pool_scale,
    delta_gain,
    w_out_pool,
    w_out_delta,
):
    n_sp, n_fs, n_tp = (lax.axis_size(a) for a in ("sp", "fs", "tp"))
    weights = (w_key, w_query, w_value, w_pool_in, w_gate, w_out_pool, w_out_delta)
    rows, width = tokens.shape
    depth, cols = w_key.shape
    heads = a_log.shape[0]
    head_dim = cols // heads
    length = n_tp * rows
    count = len(weights)
    lanes = 128
    lane = lax.axis_index("tp")

    def own(w):
        return lax.dynamic_slice_in_dim(w, lane * heads, heads, 1)

    def wide(x):
        return jnp.pad(x, ((0, 0), (0, lanes - x.shape[1])))

    w_bd = wide(jnp.concatenate([own(w_decay), own(w_beta)], axis=1))
    slots = max(1, 2 ** len(share_bits(n_fs)) - 1)
    side = max(1, n_tp - 1)
    dma = pltpu.SemaphoreType.DMA
    vmem, anywhere = pl.BlockSpec(memory_space=pltpu.VMEM), pl.BlockSpec(memory_space=pl.ANY)
    return pl.pallas_call(
        functools.partial(mixer_kernel, n_sp, n_fs, n_tp),
        out_shape=jax.ShapeDtypeStruct((rows, width), bf16),
        in_specs=[anywhere] + [vmem] * 8 + [anywhere] * count,
        out_specs=vmem,
        scratch_shapes=[
            pltpu.VMEM((halo + length, width), bf16),
            pltpu.VMEM((halo + length, width), bf16),
            pltpu.VMEM((count, n_sp, depth, cols), bf16),
            pltpu.VMEM((5, halo + length, cols), f32),
            pltpu.VMEM((length, cols), bf16),
            pltpu.VMEM((length, cols), bf16),
            pltpu.VMEM((heads, length, 2 * head_dim), f32),
            pltpu.VMEM((heads, head_dim, 2 * head_dim), f32),
            pltpu.VMEM((heads, head_dim, head_dim), bf16),
            pltpu.VMEM((heads, head_dim, head_dim), bf16),
            pltpu.VMEM((n_sp, length, cols), bf16),
            pltpu.VMEM((n_sp, n_tp, rows, cols), bf16),
            dma((count + 1,)), dma((side,)), dma((side,)), dma((n_tp,)), dma((n_tp,)),
            dma((count, n_sp, 2)), dma((count, n_sp)), dma((count, n_sp, slots)), dma((count, n_sp, slots)),
            dma((heads,)), dma((heads,)), dma((n_sp, side)), dma((n_sp, side)),
        ],
        compiler_params=pltpu.CompilerParams(collective_id=0, has_side_effects=True, vmem_limit_bytes=56 << 20),
    )(tokens, norm_gain.reshape(1, -1), w_bd, conv_weight, wide(a_log.reshape(1, -1)), wide(decay_extra), w_mix,
      pool_scale.reshape(1, -1), delta_gain.reshape(1, -1), *weights)


def solution(mesh):
    placed = (
        P(("fs", "sp", "tp"), None),
        P(),
        P("sp", "tp"),
        P("sp", "tp"),
        P("sp", "tp"),
        P("sp", "tp"),
        P("sp", "tp"),
        P(),
        P(),
        P(None, None, "tp"),
        P("tp"),
        P(("fs", "sp"), "tp"),
        P("tp", None, None),
        P("tp"),
        P(),
        P("tp", "sp"),
        P("tp", "sp"),
    )
    return jax.shard_map(
        per_device,
        mesh=mesh,
        in_specs=placed,
        out_specs=P(("fs", "sp", "tp"), None),
        check_vma=False,
    )
```
